32 devices in a mesh: grp: 2 (over x), ep: 16 (over z, y, core).
Axes of the slice: x: 2, y: 2, z: 4, core: 2. Of those that a mesh axis runs over, the one named last changes fastest.
Arguments:
- tokens: bfloat16 [384, 2048], P(('grp', 'ep')), parts along dimension 0, may hold values from -6 to 6
- norm_gain: float32 [2048], replicated, may hold values from 0.1 to 1.9
- query_weight: bfloat16 [2048, 512], P('ep'), may hold values from -0.125 to 0.125
- key_weight: bfloat16 [2048, 512], P('ep'), may hold values from -0.125 to 0.125
- value_weight: bfloat16 [2048, 512], P('ep'), may hold values from -0.125 to 0.125
- outgate_weight: bfloat16 [2048, 512], P('ep'), may hold values from -0.125 to 0.125
- ingate_weight: bfloat16 [2048, 4], P('ep'), may hold values from -0.125 to 0.125
- forget_weight: bfloat16 [2048, 4], P('ep'), may hold values from -0.125 to 0.125
- ingate_bias: float32 [4], replicated, may hold values from -1 to 1
- forget_bias: float32 [4], replicated, may hold values from 0.5 to 4
- memory: float32 [384, 4, 128, 128], P(('grp', 'ep')), parts along dimension 0, may hold values from -4 to 4
- normalizer: float32 [384, 4, 128], P(('grp', 'ep')), parts along dimension 0, may hold values from -4 to 4
- stabilizer: float32 [384, 4], P(('grp', 'ep')), parts along dimension 0, may hold values from -1 to 2
- mixer_weight: bfloat16 [512, 2048], P(None, 'ep'), may hold values from -0.25 to 0.25
- moe_gain: float32 [2048], replicated, may hold values from 0.1 to 1.9
- expert_gate: bfloat16 [16, 2048, 512], P('ep'), may hold values from -0.125 to 0.125
- expert_up: bfloat16 [16, 2048, 512], P('ep'), may hold values from -0.125 to 0.125
- expert_down: bfloat16 [16, 512, 2048], P('ep'), may hold values from -0.25 to 0.25
- expert_index: int32 [384, 6], P(('grp', 'ep')), parts along dimension 0, may hold values from 0 to 15, as said below
- route_weights: float32 [384, 6], P(('grp', 'ep')), parts along dimension 0, may hold values from 0.1 to 1
Outputs:
- layer_out: bfloat16 [384, 2048], P(('grp', 'ep')), parts along dimension 0
- new_memory: float32 [384, 4, 128, 128], P(('grp', 'ep')), parts along dimension 0
- new_normalizer: float32 [384, 4, 128], P(('grp', 'ep')), parts along dimension 0
- new_stabilizer: float32 [384, 4], P(('grp', 'ep')), parts along dimension 0
The draws below stay inside these ranges and needn't reach their ends.
There are 2 independent parts, one for each index of `grp`. The reference program is written for one: setup_inputs(seed, part) draws one part's arguments, and reference() takes and returns one part's arrays. A program takes and returns all parts, laid end to end along the dimension named above; an argument that names none is the same for every part. Nothing has to cross between parts.
Inputs may be any that keep to these rules, and one draw needn't show every extreme that they name: `expert_index`: experts 0 to 15 form two groups of 8 consecutive numbers; each row names 6 different experts of one group. Among the 12 rows of one device at most 5 name one expert, and in every device some expert is named by exactly 5 of them.
All inputs are finite; a program needn't handle non-finite values.
Results may differ from the reference program's by a relative error of at most 0.013.
Values may be sent and summed in bfloat16 or wider, within the bound.
A program may use at most 128 MiB of HBM per device.

```python
import math
import jax
import jax.numpy as jnp
from jax import lax

D = 2048
M_HEADS = 4
M_HEAD_DIM = 128
M_WIDTH = 512
D_EXPERT = 512
TOP_K = 6
EXPERTS = 16
SEQ_DEV = 12
TOKENS = 192
CAP = 5
N_EP = 16


def draw_expert_index(key, part):
    blocks = TOKENS // SEQ_DEV
    group_size = EXPERTS // 2
    offsets = jax.random.randint(jax.random.fold_in(key, 21), (blocks, 2), 0, group_size)
    flips = jax.random.randint(jax.random.fold_in(key, 22), (blocks, 1), 0, 2)
    within = jnp.arange(SEQ_DEV, dtype=jnp.int32)
    parity = within % 2
    groups = (parity[None, :] + flips) % 2
    position = within // 2
    starts = jnp.take_along_axis(offsets, groups, axis=1) + position[None, :] * TOP_K
    steps_k = jnp.arange(TOP_K, dtype=jnp.int32)
    chosen = groups[:, :, None] * group_size + (starts[:, :, None] + steps_k[None, None, :]) % group_size
    block_keys = jax.random.split(jax.random.fold_in(key, 23), blocks)
    orders = jax.vmap(lambda single: jax.random.permutation(single, SEQ_DEV))(block_keys)
    chosen = jnp.take_along_axis(chosen, orders[:, :, None], axis=1)
    return chosen.reshape(TOKENS, TOP_K).astype(jnp.int32)


def block_scale(stream_key, dims, pieces, least, top_value):
    loudness, own = 1.0, jax.random.fold_in(stream_key, 6)
    for dim, shards_of in pieces:
        steps = jnp.exp(jax.random.uniform(jax.random.fold_in(own, dim), (shards_of,), jnp.float32, least / len(pieces), top_value / len(pieces)))
        loudness = loudness * jnp.repeat(steps, dims[dim] // shards_of).reshape([-1 if axis == dim else 1 for axis in range(len(dims))])
    return loudness


def gaussian(rng, dims, spread, most, pieces=(), kind=jnp.bfloat16):
    level = block_scale(rng, dims, pieces, -0.22, 0.18) if pieces else 1.0
    values = jax.random.normal(rng, dims, jnp.float32) * spread * level
    return jnp.minimum(jnp.maximum(values, -most), most).astype(kind)


def setup_inputs(seed: int = 0, part: int = 0) -> dict:
    streams_of = jax.random.split(jax.random.key(seed), 21)
    own_keys = jax.random.split(jax.random.fold_in(streams_of[20], part), 21)
    tokens = gaussian(own_keys[0], (TOKENS, D), 1.0, 6.0, ((0, 16),))
    norm_gain = jnp.clip(1.0 + 0.18 * jax.random.normal(streams_of[1], (D,), jnp.float32), 0.1, 1.9)
    query_weight = gaussian(streams_of[2], (D, M_WIDTH), D ** -0.5, 0.125, ((0, 16),))
    key_weight = gaussian(streams_of[3], (D, M_WIDTH), D ** -0.5, 0.125, ((0, 16),))
    value_weight = gaussian(streams_of[4], (D, M_WIDTH), D ** -0.5, 0.125, ((0, 16),))
    outgate_weight = gaussian(streams_of[5], (D, M_WIDTH), D ** -0.5, 0.125, ((0, 16),))
    ingate_weight = gaussian(streams_of[6], (D, M_HEADS), D ** -0.5, 0.125, ((0, 16),))
    forget_weight = gaussian(streams_of[7], (D, M_HEADS), D ** -0.5, 0.125, ((0, 16),))
    ingate_bias = jnp.clip(jax.random.uniform(streams_of[8], (M_HEADS,), jnp.float32, -1.0, 1.0), -1.0, 1.0)
    forget_bias = jnp.clip(jax.random.uniform(streams_of[9], (M_HEADS,), jnp.float32, 0.5, 4.0), 0.5, 4.0)
    memory = gaussian(own_keys[10], (TOKENS, M_HEADS, M_HEAD_DIM, M_HEAD_DIM), 0.3, 4.0, ((0, 16),), jnp.float32)
    normalizer = gaussian(own_keys[11], (TOKENS, M_HEADS, M_HEAD_DIM), 0.3, 4.0, ((0, 16),), jnp.float32)
    stabilizer = jnp.clip(-1.0 + 3.0 * jax.random.uniform(own_keys[12], (TOKENS, M_HEADS), jnp.float32) ** block_scale(own_keys[12], (TOKENS, M_HEADS), ((0, 16),), -0.2, 0.2), -1.0, 2.0)
    mixer_weight = gaussian(streams_of[13], (M_WIDTH, D), M_WIDTH ** -0.5, 0.25, ((1, 16),))
    moe_gain = jnp.clip(1.0 + 0.18 * jax.random.normal(streams_of[14], (D,), jnp.float32), 0.1, 1.9)
    expert_gate = gaussian(streams_of[15], (EXPERTS, D, D_EXPERT), D ** -0.5, 0.125, ((0, 16),))
    expert_up = gaussian(streams_of[16], (EXPERTS, D, D_EXPERT), D ** -0.5, 0.125, ((0, 16),))
    expert_down = gaussian(streams_of[17], (EXPERTS, D_EXPERT, D), D_EXPERT ** -0.5, 0.25, ((0, 16),))
    expert_index = draw_expert_index(jax.random.fold_in(jax.random.fold_in(streams_of[20], part), 71), part)
    route_weights = jnp.clip(jnp.exp(math.log(1.0) - 2.3025851 * jax.random.uniform(own_keys[19], (TOKENS, TOP_K), jnp.float32) ** block_scale(own_keys[19], (TOKENS, TOP_K), ((0, 16),), -0.2, 0.2)), 0.1, 1.0)
    return {"tokens": tokens, "norm_gain": norm_gain, "query_weight": query_weight, "key_weight": key_weight, "value_weight": value_weight, "outgate_weight": outgate_weight, "ingate_weight": ingate_weight, "forget_weight": forget_weight, "ingate_bias": ingate_bias, "forget_bias": forget_bias, "memory": memory, "normalizer": normalizer, "stabilizer": stabilizer, "mixer_weight": mixer_weight, "moe_gain": moe_gain, "expert_gate": expert_gate, "expert_up": expert_up, "expert_down": expert_down, "expert_index": expert_index, "route_weights": route_weights}


EPS = 1e-06

def rms_normed(values, gain):
    scale = lax.rsqrt(lax.optimization_barrier(jnp.mean(values * values, axis=-1, keepdims=True)) + EPS)
    return values * scale * gain

def reference(tokens, norm_gain, query_weight, key_weight, value_weight, outgate_weight, ingate_weight, forget_weight, ingate_bias, forget_bias, memory, normalizer, stabilizer, mixer_weight, moe_gain, expert_gate, expert_up, expert_down, expert_index, route_weights):
    f32 = jnp.float32
    bf16 = jnp.bfloat16
    stream = tokens.astype(f32)
    normed = rms_normed(stream, norm_gain).astype(bf16)

    def project(weight):
        return jnp.dot(normed, weight, preferred_element_type=f32)
    queries = project(query_weight).astype(bf16)
    key_rows = project(key_weight).astype(bf16)
    value_rows = project(value_weight).astype(bf16)
    outgate = project(outgate_weight).astype(bf16)
    ingate_pre = project(ingate_weight) + ingate_bias
    forget_pre = project(forget_weight) + forget_bias
    shape = (TOKENS, M_HEADS, M_HEAD_DIM)
    query_heads = queries.astype(f32).reshape(shape)
    key_heads = key_rows.astype(f32).reshape(shape) * M_HEAD_DIM ** (-0.5)
    value_heads = value_rows.astype(f32).reshape(shape)
    log_forget = jax.nn.log_sigmoid(forget_pre)
    new_stabilizer = jnp.maximum(log_forget + stabilizer, ingate_pre)
    keep = jnp.exp(log_forget + stabilizer - new_stabilizer)
    write = jnp.exp(ingate_pre - new_stabilizer)
    new_memory = keep[..., None, None] * memory + write[..., None, None] * key_heads[..., :, None] * value_heads[..., None, :]
    new_normalizer = keep[..., None] * normalizer + write[..., None] * key_heads
    numer = jnp.einsum('thd,thde->the', query_heads, new_memory, precision=lax.Precision.HIGHEST)
    denom = lax.optimization_barrier(jnp.sum(query_heads * new_normalizer, axis=-1))
    hidden = numer / jnp.maximum(jnp.abs(denom), 1.0)[..., None]
    cell_out = (hidden.reshape(TOKENS, M_WIDTH) * jax.nn.sigmoid(outgate.astype(f32))).astype(bf16)
    mixed = jnp.dot(cell_out, mixer_weight, preferred_element_type=f32).astype(bf16)
    resid = stream + mixed.astype(f32)
    moe_in = rms_normed(resid, moe_gain).astype(bf16)
    limit = N_EP * CAP
    padded_in = jnp.concatenate([moe_in, jnp.zeros((1, D), bf16)], axis=0)

    def one_expert(total, expert):
        chosen = expert_index == expert
        weight = lax.optimization_barrier(jnp.sum(jnp.where(chosen, route_weights, 0.0), axis=1))
        rows = jnp.nonzero(jnp.any(chosen, axis=1), size=limit, fill_value=TOKENS)[0].astype(jnp.int32)
        picked = padded_in[rows]
        gate = jnp.dot(picked, expert_gate[expert], preferred_element_type=f32)
        upward = jnp.dot(picked, expert_up[expert], preferred_element_type=f32)
        inner = (jax.nn.silu(gate) * upward).astype(bf16)
        result = jnp.dot(inner, expert_down[expert], preferred_element_type=f32).astype(bf16)
        padded_weight = jnp.concatenate([weight, jnp.zeros((1,), f32)])
        total = total.at[rows].add(result.astype(f32) * padded_weight[rows][:, None])
        return (total, None)
    start = jnp.zeros((TOKENS + 1, D), f32)
    total, unused = lax.scan(one_expert, start, jnp.arange(EXPERTS, dtype=jnp.int32))
    layer_out = (resid + total[:TOKENS]).astype(bf16)
    return (layer_out, new_memory, new_normalizer, new_stabilizer)
```

```python
import functools

import jax
import jax.numpy as jnp
from jax import lax
from jax.experimental import pallas as pl
from jax.experimental.pallas import tpu as pltpu
from jax.sharding import PartitionSpec as P

M_HEAD_DIM = 128
LANES = 128
HALF = 64
EPS = 1e-06
f32 = jnp.float32
bf16 = jnp.bfloat16


def rms_normed(values, gain):
    scale = lax.rsqrt(jnp.mean(values * values, axis=-1, keepdims=True) + EPS)
    return values * scale * gain


def remote(src, dst, send_sem, recv_sem, device):
    return pltpu.make_async_remote_copy(
        src_ref=src,
        dst_ref=dst,
        send_sem=send_sem,
        recv_sem=recv_sem,
        device_id={"ep": device},
        device_id_type=pl.DeviceIdType.MESH,
    )


def loop(low, high, body):
    def step(index, carry):
        body(index)
        return carry

    lax.fori_loop(low, high, step, 0)


def split_lanes(values):
    lane = lax.broadcasted_iota(jnp.int32, values.shape, 1)
    high = values.astype(bf16).astype(f32)
    return jnp.where(lane < HALF, high, values - high).astype(bf16)


def layer_kernel(
    n,
    seq,
    group_width,
    tokens,
    norm_gain,
    ingate_weight,
    forget_weight,
    ingate_bias,
    forget_bias,
    normalizer,
    stabilizer,
    moe_gain,
    expert_index,
    route_weights,
    query_weight,
    key_weight,
    value_weight,
    outgate_weight,
    memory,
    mixer_weight,
    expert_gate,
    expert_up,
    expert_down,
    layer_out,
    new_normalizer,
    new_stabilizer,
    new_memory,
    proj_w,
    gate_w,
    mem,
    mix_w,
    gate_e,
    up_e,
    down_e,
    normed,
    normed_cols,
    part,
    pair_send,
    pair_recv,
    sum_send,
    sum_recv,
    key_t,
    query_t,
    value_rows,
    keep_rows,
    numer,
    cells,
    mixed_send,
    mixed,
    resid_rows,
    packed,
    routed,
    outcome,
    back_pair_send,
    back_pair_recv,
    back_send,
    back_recv,
    load_sem,
    store_sem,
    send_a,
    recv_a,
    send_b,
    recv_b,
    send_c,
    recv_c,
    send_d,
    recv_d,
    send_e,
    recv_e,
    send_f,
    recv_f,
    send_g,
    recv_g,
    send_h,
    recv_h,
    send_i,
    recv_i,
):
    me = lax.axis_index("ep")
    core = lax.rem(me, 2)
    chip = me // 2
    partner = me + 1 - 2 * core
    chips = n // 2
    width = proj_w.shape[1] // 4
    heads = mem.shape[1]
    model = tokens.shape[1]
    slots = packed.shape[1]

    loads = [
        pltpu.make_async_copy(source, target, load_sem.at[index])
        for index, (source, target) in enumerate(
            (
                (query_weight, proj_w.at[:, pl.ds(0, width)]),
                (key_weight, proj_w.at[:, pl.ds(width, width)]),
                (value_weight, proj_w.at[:, pl.ds(2 * width, width)]),
                (outgate_weight, proj_w.at[:, pl.ds(3 * width, width)]),
                (memory, mem),
                (mixer_weight, mix_w),
                (expert_gate, gate_e),
                (expert_up, up_e),
                (expert_down, down_e),
            )
        )
    ]
    for load in loads:
        load.start()

    barrier = pltpu.get_barrier_semaphore()

    def greet(k):
        pl.semaphore_signal(
            barrier,
            inc=1,
            device_id={"ep": lax.rem(me + k, n)},
            device_id_type=pl.DeviceIdType.MESH,
        )

    loop(1, n, greet)

    stream = tokens[...].astype(f32)
    depth = normed_cols.shape[2]
    scaled = rms_normed(stream, norm_gain[...]).astype(bf16)
    normed[:, pl.ds(seq, 16 - seq), :] = jnp.zeros((n, 16 - seq, depth), bf16)
    for d in range(n):
        normed[d, pl.ds(0, seq), :] = scaled[:, d * depth : (d + 1) * depth]
    gate_w[...] = jnp.zeros(gate_w.shape, bf16)
    for base in (0, HALF):
        gate_w[:, base : base + heads] = ingate_weight[...]
        gate_w[:, base + heads : base + 2 * heads] = forget_weight[...]

    pl.semaphore_wait(barrier, n - 1)

    def send_cols(k):
        to = lax.rem(me + k, n)
        remote(normed.at[to], normed_cols.at[me], send_a.at[to], recv_a.at[me], to).start()

    def wait_cols(k):
        of = lax.rem(me + k, n)
        remote(normed.at[of], normed_cols.at[of], send_a.at[of], recv_a.at[of], of).wait()

    loop(1, n, send_cols)
    normed_cols[me] = normed[me]
    for load in loads[:4]:
        load.wait()
    loop(1, n, wait_cols)

    rows = normed_cols[...].reshape(n * 16, depth)
    for piece in range(4):
        columns = slice(piece * width, (piece + 1) * width)
        block = jnp.dot(rows, proj_w[:, columns], preferred_element_type=f32)
        part[:, :, columns] = block.reshape(n, 16, width)
    gates = jnp.dot(rows, gate_w[...], preferred_element_type=f32)
    part[:, :, 4 * width :] = gates.reshape(n, 16, LANES)

    def pack_sums(values):
        return values[:, : 4 * width].astype(bf16), split_lanes(values[:, 4 * width :])

    def unpack_sums(values):
        narrow = values[:, 4 * width :]
        whole = narrow + pltpu.roll(narrow, HALF, 1)
        return jnp.concatenate([values[:, : 4 * width], whole], axis=1)

    def pair_copy(j):
        return remote(
            pair_send.at[j], pair_recv.at[j], send_b.at[j], recv_b.at[j], partner
        )

    def send_pair(k):
        j = lax.rem(chip + k, chips)
        wide, narrow = pack_sums(part[2 * j + 1 - core])
        pair_send[j, :, : 4 * width] = wide
        pair_send[j, :, 4 * width :] = narrow
        pair_copy(j).start()

    loop(1, chips + 1, send_pair)

    def sum_copy(j, slot):
        return remote(
            sum_send.at[j],
            sum_recv.at[slot],
            send_c.at[j],
            recv_c.at[slot],
            2 * j + core,
        )

    def send_sum(k):
        j = lax.rem(chip + k, chips)
        pair_copy(j).wait()
        wide, narrow = pack_sums(part[2 * j + core] + unpack_sums(pair_recv[j].astype(f32)))
        sum_send[j, :, : 4 * width] = wide
        sum_send[j, :, 4 * width :] = narrow
        sum_copy(j, chip).start()

    loop(1, chips, send_sum)
    pair_copy(chip).wait()
    own = part[me] + unpack_sums(pair_recv[chip].astype(f32))

    def wait_sum(k, total):
        j = lax.rem(chip + k, chips)
        sum_copy(j, j).wait()
        return total + sum_recv[j].astype(f32)

    others = lax.fori_loop(1, chips, wait_sum, jnp.zeros(own.shape, f32))
    sums = (own + unpack_sums(others))[:seq]

    scale = M_HEAD_DIM ** (-0.5)
    gates = sums[:, 4 * width : 4 * width + 2 * heads]
    ingate_pre = gates[:, :heads] + ingate_bias[...]
    forget_pre = gates[:, heads:] + forget_bias[...]
    log_forget = jnp.minimum(forget_pre, 0.0) - jnp.log1p(jnp.exp(-jnp.abs(forget_pre)))
    stable = jnp.maximum(log_forget + stabilizer[...], ingate_pre)
    new_stabilizer[...] = stable
    keep = jnp.exp(log_forget + stabilizer[...] - stable)
    write = jnp.exp(ingate_pre - stable)
    rank = (M_HEAD_DIM, M_HEAD_DIM)
    unit = (
        lax.broadcasted_iota(jnp.int32, rank, 0) == lax.broadcasted_iota(jnp.int32, rank, 1)
    ).astype(bf16)
    contract = (((1,), (1,)), ((), ()))
    denoms = []
    for h in range(heads):
        lanes = slice(h * M_HEAD_DIM, (h + 1) * M_HEAD_DIM)
        query = sums[:, 0 * width :][:, lanes].astype(bf16)
        key = sums[:, 1 * width :][:, lanes].astype(bf16)
        value = sums[:, 2 * width :][:, lanes].astype(bf16)
        query_t[h] = lax.dot_general(unit, query, contract, preferred_element_type=f32)
        key_t[h] = lax.dot_general(unit, key, contract, preferred_element_type=f32) * scale
        value_rows[h] = value.astype(f32) * write[:, h : h + 1]
        keep_rows[h] = jnp.broadcast_to(keep[:, h : h + 1], (seq, M_HEAD_DIM))
        fresh = (
            keep[:, h : h + 1] * normalizer[:, h, :]
            + write[:, h : h + 1] * key.astype(f32) * scale
        )
        new_normalizer[:, h, :] = fresh
        denoms.append(jnp.sum(query.astype(f32) * fresh, axis=-1, keepdims=True))
    loads[4].wait()

    def one_head(h):
        for t in range(seq):
            fresh = (
                keep_rows[h, t : t + 1, :] * mem[t, h]
                + key_t[h, :, t : t + 1] * value_rows[h, t : t + 1, :]
            )
            mem[t, h] = fresh
            numer[h, t : t + 1, :] = jnp.sum(
                query_t[h, :, t : t + 1] * fresh, axis=0, keepdims=True
            )

    loop(0, heads, one_head)
    memory_store = pltpu.make_async_copy(mem, new_memory, store_sem.at[0])
    memory_store.start()
    outgate = sums[:, 3 * width : 4 * width].astype(bf16).astype(f32)
    opened = jax.nn.sigmoid(outgate)
    cells[me] = jnp.zeros(cells.shape[1:], bf16)
    for h in range(heads):
        lanes = slice(h * M_HEAD_DIM, (h + 1) * M_HEAD_DIM)
        hidden = numer[h] / jnp.maximum(jnp.abs(denoms[h]), 1.0)
        cells[me, pl.ds(0, seq), lanes] = (hidden * opened[:, lanes]).astype(bf16)

    def cell_copy(to, slot):
        return remote(cells.at[slot], cells.at[slot], send_d.at[to], recv_d.at[slot], to)

    loop(1, n, lambda k: cell_copy(lax.rem(me + k, n), me).start())
    loads[5].wait()

    def wait_cell(k):
        of = lax.rem(me + k, n)
        cell_copy(of, of).wait_recv()

    loop(1, n, wait_cell)
    mixes = jnp.dot(
        cells[...].reshape(n * 16, width), mix_w[...], preferred_element_type=f32
    ).astype(bf16)
    mixed_send[...] = mixes.reshape(n, 16, depth)

    def mixed_copy(to, slot):
        return remote(mixed_send.at[to], mixed.at[slot], send_e.at[to], recv_e.at[slot], to)

    loop(1, n, lambda k: mixed_copy(lax.rem(me + k, n), me).start())
    mixed[me] = mixed_send[me]

    index = expert_index[...]
    group = (index[:, 0:1] >= group_width).astype(jnp.int32)
    lane = lax.broadcasted_iota(jnp.int32, (seq, LANES), 1)
    named = group * group_width + jnp.where(lane < HALF, lane, lane - HALF)
    inside = jnp.where(lane < HALF, lane, lane - HALF) < group_width
    shares = jnp.zeros((seq, LANES), f32)
    for k in range(index.shape[1]):
        hit = (index[:, k : k + 1] == named) & inside
        shares = shares + jnp.where(hit, route_weights[:, k : k + 1], 0.0)
    shares = split_lanes(shares)
    square = (seq, seq)
    earlier = (
        lax.broadcasted_iota(jnp.int32, square, 1) < lax.broadcasted_iota(jnp.int32, square, 0)
    ).astype(f32)
    second = group.astype(f32)
    before_second = jnp.dot(
        earlier, jnp.broadcast_to(second, (seq, LANES)), preferred_element_type=f32
    )[:, 0:1]
    order = lax.broadcasted_iota(jnp.int32, (seq, 1), 0).astype(f32)
    place = jnp.where(second > 0.5, before_second + slots, order - before_second)
    spread = (
        place == lax.broadcasted_iota(jnp.int32, (seq, 2 * slots), 1).astype(f32)
    ).astype(bf16)

    def wait_mixed(k):
        of = lax.rem(me + k, n)
        mixed_copy(of, of).wait_recv()

    loop(1, n, wait_mixed)
    for d in range(n):
        columns = slice(d * depth, (d + 1) * depth)
        resid_rows[:, columns] = tokens[:, columns].astype(f32) + mixed[
            d, pl.ds(0, seq), :
        ].astype(f32)
    resid = resid_rows[...]
    moe_in = rms_normed(resid, moe_gain[...]).astype(bf16)
    first = (((0,), (0,)), ((), ()))
    for g in range(2):
        mine = spread[:, g * slots : (g + 1) * slots]
        packed[g, :, :model] = lax.dot_general(
            mine, moe_in, first, preferred_element_type=f32
        ).astype(bf16)
        packed[g, :, model:] = lax.dot_general(
            mine, shares, first, preferred_element_type=f32
        ).astype(bf16)

    half_chips = chips // 2

    def route_copy(j, slot):
        return remote(
            packed.at[j // half_chips],
            routed.at[2 * slot + core],
            send_f.at[j],
            recv_f.at[slot],
            2 * j + core,
        )

    def relay_copy(slot, side):
        return remote(
            routed.at[2 * slot + side],
            routed.at[2 * slot + side],
            send_g.at[slot],
            recv_g.at[slot],
            partner,
        )

    loop(1, chips, lambda k: route_copy(lax.rem(chip + k, chips), chip).start())
    routed[me] = packed[chip // half_chips]
    relay_copy(chip, core).start()

    def relay(k):
        slot = lax.rem(chip + chips - k, chips)
        route_copy(slot, slot).wait_recv()
        relay_copy(slot, core).start()

    loop(1, chips, relay)
    for load in loads[6:]:
        load.wait()
    loop(0, chips, lambda slot: relay_copy(slot, 1 - core).wait_recv())

    arrived = routed[...].reshape(n * slots, model + LANES)
    rows = arrived[:, :model]
    gate = jnp.dot(rows, gate_e[0], preferred_element_type=f32)
    upward = jnp.dot(rows, up_e[0], preferred_element_type=f32)
    inner = (gate * jax.nn.sigmoid(gate) * upward).astype(bf16)
    spot = lax.rem(me, group_width)
    lane = lax.broadcasted_iota(jnp.int32, (n * slots, LANES), 1)
    share = jnp.sum(
        jnp.where(
            (lane == spot) | (lane == spot + HALF), arrived[:, model:].astype(f32), 0.0
        ),
        axis=1,
        keepdims=True,
    )
    result = jnp.dot(inner, down_e[0], preferred_element_type=f32).astype(bf16).astype(f32)
    outcome[...] = (result * share).reshape(n, slots, model)

    def back_pair(j):
        return remote(
            back_pair_send.at[j], back_pair_recv.at[j], send_h.at[j], recv_h.at[j], partner
        )

    def send_back_pair(k):
        j = lax.rem(chip + k, chips)
        back_pair_send[j] = outcome[2 * j + 1 - core].astype(bf16)
        back_pair(j).start()

    loop(1, chips + 1, send_back_pair)

    def back_copy(j, slot):
        return remote(
            back_send.at[j], back_recv.at[slot], send_i.at[j], recv_i.at[slot], 2 * j + core
        )

    def send_back(k):
        j = lax.rem(chip + k, chips)
        back_pair(j).wait()
        back_send[j] = (outcome[2 * j + core] + back_pair_recv[j].astype(f32)).astype(bf16)
        back_copy(j, chip).start()

    loop(1, chips, send_back)
    back_pair(chip).wait()
    back_recv[chip] = (outcome[me] + back_pair_recv[chip].astype(f32)).astype(bf16)

    def wait_back(k):
        j = lax.rem(chip + k, chips)
        back_copy(j, j).wait()

    loop(1, chips, wait_back)
    combined = resid
    for g in range(2):
        base = g * half_chips
        total = lax.fori_loop(
            1,
            half_chips,
            lambda j, carry: carry + back_recv[base + j].astype(f32),
            back_recv[base].astype(f32),
        )
        high = total.astype(bf16)
        low = (total - high.astype(f32)).astype(bf16)
        mine = spread[:, g * slots : (g + 1) * slots]
        combined = combined + jnp.dot(mine, high, preferred_element_type=f32)
        combined = combined + jnp.dot(mine, low, preferred_element_type=f32)
    layer_out[...] = combined.astype(bf16)

    def sent(k):
        to = lax.rem(me + k, n)
        cell_copy(to, me).wait_send()
        mixed_copy(to, me).wait_send()

    loop(1, n, sent)
    loop(1, chips, lambda k: route_copy(lax.rem(chip + k, chips), chip).wait_send())
    loop(0, chips, lambda slot: relay_copy(slot, core).wait_send())
    memory_store.wait()


def on_device(
    tokens,
    norm_gain,
    query_weight,
    key_weight,
    value_weight,
    outgate_weight,
    ingate_weight,
    forget_weight,
    ingate_bias,
    forget_bias,
    memory,
    normalizer,
    stabilizer,
    mixer_weight,
    moe_gain,
    expert_gate,
    expert_up,
    expert_down,
    expert_index,
    route_weights,
):
    n = lax.axis_size("ep")
    seq, model = tokens.shape
    depth, width = query_weight.shape
    heads = ingate_bias.shape[0]
    hidden = expert_gate.shape[2]
    chosen_k = expert_index.shape[1]
    group_width = n // 2
    capacity = max(2, ((seq + 1) // 2 * chosen_k + group_width - 1) // group_width)
    most = min(seq, group_width * capacity // chosen_k)
    slots = (most + 7) // 8 * 8
    chips = n // 2
    total = 4 * width + LANES
    vmem = pl.BlockSpec(memory_space=pltpu.VMEM)
    hbm = pl.BlockSpec(memory_space=pl.ANY)
    dma = pltpu.SemaphoreType.DMA
    V = pltpu.VMEM
    wide, narrow = (n,), (chips,)
    return_shapes = (
        jax.ShapeDtypeStruct((seq, model), bf16),
        jax.ShapeDtypeStruct(normalizer.shape, f32),
        jax.ShapeDtypeStruct(stabilizer.shape, f32),
        jax.ShapeDtypeStruct(memory.shape, f32),
    )
    out, norm_out, stab_out, mem_out = pl.pallas_call(
        functools.partial(layer_kernel, n, seq, group_width),
        out_shape=return_shapes,
        in_specs=[vmem] * 11 + [hbm] * 9,
        out_specs=(vmem, vmem, vmem, hbm),
        scratch_shapes=[
            V((depth, 4 * width), bf16),
            V((depth, LANES), bf16),
            V(memory.shape, f32),
            V(mixer_weight.shape, bf16),
            V(expert_gate.shape, bf16),
            V(expert_up.shape, bf16),
            V(expert_down.shape, bf16),
            V((n, 16, depth), bf16),
            V((n, 16, depth), bf16),
            V((n, 16, total), f32),
            V((chips, 16, total), bf16),
            V((chips, 16, total), bf16),
            V((chips, 16, total), bf16),
            V((chips, 16, total), bf16),
            V((heads, M_HEAD_DIM, seq), f32),
            V((heads, M_HEAD_DIM, seq), f32),
            V((heads, seq, M_HEAD_DIM), f32),
            V((heads, seq, M_HEAD_DIM), f32),
            V((heads, seq, M_HEAD_DIM), f32),
            V((n, 16, width), bf16),
            V((n, 16, depth), bf16),
            V((n, 16, depth), bf16),
            V((seq, model), f32),
            V((2, slots, model + LANES), bf16),
            V((n, slots, model + LANES), bf16),
            V((n, slots, model), f32),
            V((chips, slots, model), bf16),
            V((chips, slots, model), bf16),
            V((chips, slots, model), bf16),
            V((chips, slots, model), bf16),
            dma((9,)),
            dma((1,)),
        ]
        + [dma(wide), dma(wide)]
        + [dma(narrow), dma(narrow)] * 2
        + [dma(wide), dma(wide)] * 2
        + [dma(narrow), dma(narrow)] * 4,
        compiler_params=pltpu.CompilerParams(
            collective_id=0, has_side_effects=True, vmem_limit_bytes=60 * 1024 * 1024
        ),
    )(
        tokens,
        norm_gain.reshape(1, model),
        ingate_weight,
        forget_weight,
        ingate_bias.reshape(1, heads),
        forget_bias.reshape(1, heads),
        normalizer,
        stabilizer,
        moe_gain.reshape(1, model),
        expert_index,
        route_weights,
        query_weight,
        key_weight,
        value_weight,
        outgate_weight,
        memory,
        mixer_weight,
        expert_gate,
        expert_up,
        expert_down,
    )
    return (out, mem_out, norm_out, stab_out)


def solution(mesh):
    return jax.shard_map(
        on_device,
        mesh=mesh,
        in_specs=(
            P(("grp", "ep"), None),
            P(),
            P("ep", None),
            P("ep", None),
            P("ep", None),
            P("ep", None),
            P("ep", None),
            P("ep", None),
            P(),
            P(),
            P(("grp", "ep"), None, None, None),
            P(("grp", "ep"), None, None),
            P(("grp", "ep"), None),
            P(None, "ep"),
            P(),
            P("ep", None, None),
            P("ep", None, None),
            P("ep", None, None),
            P(("grp", "ep"), None),
            P(("grp", "ep"), None),
        ),
        out_specs=(
            P(("grp", "ep"), None),
            P(("grp", "ep"), None, None, None),
            P(("grp", "ep"), None, None),
            P(("grp", "ep"), None),
        ),
        check_vma=False,
    )
```

```python
import functools

import jax
import jax.numpy as jnp
from jax import lax
from jax.experimental import pallas as pl
from jax.experimental.pallas import tpu as pltpu
from jax.sharding import PartitionSpec as P

M_HEAD_DIM = 128
LANES = 128
HALF = 64
EPS = 1e-06
f32 = jnp.float32
bf16 = jnp.bfloat16


def rms_normed(values, gain):
    scale = lax.rsqrt(jnp.mean(values * values, axis=-1, keepdims=True) + EPS)
    return values * scale * gain


def remote(src, dst, send_sem, recv_sem, device):
    return pltpu.make_async_remote_copy(
        src_ref=src,
        dst_ref=dst,
        send_sem=send_sem,
        recv_sem=recv_sem,
        device_id={"ep": device},
        device_id_type=pl.DeviceIdType.MESH,
    )


def loop(low, high, body):
    def step(index, carry):
        body(index)
        return carry

    lax.fori_loop(low, high, step, 0)


def split_lanes(values):
    lane = lax.broadcasted_iota(jnp.int32, values.shape, 1)
    high = values.astype(bf16).astype(f32)
    return jnp.where(lane < HALF, high, values - high).astype(bf16)


def layer_kernel(
    n,
    seq,
    group_width,
    tokens,
    norm_gain,
    ingate_weight,
    forget_weight,
    ingate_bias,
    forget_bias,
    normalizer,
    stabilizer,
    moe_gain,
    expert_index,
    route_weights,
    query_weight,
    key_weight,
    value_weight,
    outgate_weight,
    memory,
    mixer_weight,
    expert_gate,
    expert_up,
    expert_down,
    layer_out,
    new_normalizer,
    new_stabilizer,
    new_memory,
    small,
    flip,
    proj_w,
    gate_w,
    mem,
    mix_w,
    gate_e,
    up_e,
    down_e,
    normed,
    normed_cols,
    part,
    pair_send,
    pair_recv,
    sum_send,
    sum_recv,
    key_t,
    query_t,
    value_rows,
    keep_rows,
    numer,
    cells,
    mixed_send,
    mixed,
    resid_rows,
    packed,
    routed,
    outcome,
    back_pair_send,
    back_pair_recv,
    back_send,
    back_recv,
    load_sem,
    store_sem,
    send_a,
    recv_a,
    send_b,
    recv_b,
    send_c,
    recv_c,
    send_d,
    recv_d,
    relay_send,
    relay_recv,
    send_e,
    recv_e,
    send_f,
    recv_f,
    send_g,
    recv_g,
    send_h,
    recv_h,
    send_i,
    recv_i,
):
    me = lax.axis_index("ep")
    core = lax.rem(me, 2)
    chip = me // 2
    partner = me + 1 - 2 * core
    chips = n // 2
    width = proj_w.shape[1] // 4
    heads = mem.shape[1]
    model = tokens.shape[1]
    slots = packed.shape[1]
    total = part.shape[2]

    loads = [
        pltpu.make_async_copy(source, target, load_sem.at[index])
        for index, (source, target) in enumerate(
            (
                (query_weight, proj_w.at[:, pl.ds(0, width)]),
                (key_weight, proj_w.at[:, pl.ds(width, width)]),
                (value_weight, proj_w.at[:, pl.ds(2 * width, width)]),
                (outgate_weight, proj_w.at[:, pl.ds(3 * width, width)]),
                (memory, mem),
                (mixer_weight, mix_w),
                (expert_gate, gate_e),
                (expert_up, up_e),
                (expert_down, down_e),
            )
        )
    ]
    for load in loads:
        load.start()

    barrier = pltpu.get_barrier_semaphore()

    def greet(k):
        pl.semaphore_signal(
            barrier,
            inc=1,
            device_id={"ep": lax.rem(me + k, n)},
            device_id_type=pl.DeviceIdType.MESH,
        )

    loop(1, n, greet)

    stream = tokens[...].astype(f32)
    depth = normed_cols.shape[2]
    scaled = rms_normed(stream, norm_gain[...]).astype(bf16)
    normed[:, pl.ds(seq, 16 - seq), :] = jnp.zeros((n, 16 - seq, depth), bf16)
    for d in range(n):
        normed[d, pl.ds(0, seq), :] = scaled[:, d * depth : (d + 1) * depth]
    gate_w[...] = jnp.zeros(gate_w.shape, f32)
    for base in (0, HALF):
        gate_w[base : base + heads, :] = ingate_weight[...].astype(f32)
        gate_w[base + heads : base + 2 * heads, :] = forget_weight[...].astype(f32)
    top = expert_index.shape[0]
    small[...] = jnp.zeros(small.shape, f32)
    small[0:heads, 0:seq] = stabilizer[...]
    small[8 : 8 + top, 0:seq] = route_weights[...]
    small[16 : 16 + top, 0:seq] = expert_index[...].astype(f32)
    flipped = small[...].T
    old_stable = flipped[:seq, 0:heads]
    route_share = flipped[:seq, 8 : 8 + top]
    index = flipped[:seq, 16 : 16 + top]

    pl.semaphore_wait(barrier, n - 1)

    def send_cols(k):
        to = lax.rem(me + k, n)
        remote(normed.at[to], normed_cols.at[me], send_a.at[to], recv_a.at[me], to).start()

    def wait_cols(k):
        of = lax.rem(me + k, n)
        remote(normed.at[of], normed_cols.at[of], send_a.at[of], recv_a.at[of], of).wait()

    loop(1, n, send_cols)
    normed_cols[me] = normed[me]
    for load in loads[:4]:
        load.wait()
    loop(1, n, wait_cols)

    rows = normed_cols[...].reshape(n * 16, depth)
    for piece in range(4):
        columns = slice(piece * width, (piece + 1) * width)
        block = jnp.dot(rows, proj_w[:, columns], preferred_element_type=f32)
        part[:, :, columns] = block.reshape(n, 16, width)
    contract = (((1,), (1,)), ((), ()))
    gates = lax.dot_general(
        rows, gate_w[...].astype(bf16), contract, preferred_element_type=f32
    )
    part[:, :, 4 * width :] = gates.reshape(n, 16, LANES)

    def pack_sums(values):
        return values[:, : 4 * width].astype(bf16), split_lanes(values[:, 4 * width :])

    def unpack_sums(values):
        narrow = values[:, 4 * width :]
        whole = narrow + pltpu.roll(narrow, HALF, 1)
        return jnp.concatenate([values[:, : 4 * width], whole], axis=1)

    tail = sum_send.shape[2] - part.shape[2]

    def fold(values):
        rest = values[8:16]
        moved = pltpu.roll(rest[:, tail:], 4, 0)
        rest = jnp.concatenate(
            [rest[:, : total - tail] + moved, rest[:, total - tail : tail]], axis=1
        )
        return values[:8], rest

    def unfold(values):
        rest = values[:, total:]
        moved = pltpu.roll(rest[:, : total - tail], 4, 0)
        return jnp.concatenate(
            [values[:, :total], jnp.concatenate([rest, moved], axis=1)], axis=0
        )

    def pair_copy(j):
        return remote(
            pair_send.at[j], pair_recv.at[j], send_b.at[j], recv_b.at[j], partner
        )

    def send_pair(k):
        j = lax.rem(chip + k, chips)
        wide, narrow = pack_sums(part[2 * j + 1 - core])
        pair_send[j, :, : 4 * width] = wide
        pair_send[j, :, 4 * width :] = narrow
        pair_copy(j).start()

    loop(1, chips + 1, send_pair)

    def sum_copy(j, slot):
        return remote(
            sum_send.at[j],
            sum_recv.at[slot],
            send_c.at[j],
            recv_c.at[slot],
            2 * j + core,
        )

    def send_sum(k):
        j = lax.rem(chip + k, chips)
        pair_copy(j).wait()
        wide, narrow = pack_sums(part[2 * j + core] + unpack_sums(pair_recv[j].astype(f32)))
        joined = jnp.concatenate([wide.astype(f32), narrow.astype(f32)], axis=1)
        head, rest = fold(joined)
        sum_send[j, :, :total] = head.astype(bf16)
        sum_send[j, :, total:] = rest.astype(bf16)
        sum_copy(j, chip).start()

    loop(1, chips, send_sum)
    pair_copy(chip).wait()
    own = part[me] + unpack_sums(pair_recv[chip].astype(f32))

    def wait_sum(k, carry):
        j = lax.rem(chip + k, chips)
        sum_copy(j, j).wait()
        return carry + sum_recv[j].astype(f32)

    others = lax.fori_loop(1, chips, wait_sum, jnp.zeros(sum_recv.shape[1:], f32))
    sums = (own + unpack_sums(unfold(others)))[:seq]

    scale = M_HEAD_DIM ** (-0.5)
    gates = sums[:, 4 * width : 4 * width + 2 * heads]
    ingate_pre = gates[:, :heads] + ingate_bias[...]
    forget_pre = gates[:, heads:] + forget_bias[...]
    log_forget = jnp.minimum(forget_pre, 0.0) - jnp.log1p(jnp.exp(-jnp.abs(forget_pre)))
    stable = jnp.maximum(log_forget + old_stable, ingate_pre)
    flip[...] = jnp.zeros(flip.shape, f32)
    flip[0:seq, 0:heads] = stable
    new_stabilizer[...] = flip[...].T[:heads, :seq]
    keep = jnp.exp(log_forget + old_stable - stable)
    write = jnp.exp(ingate_pre - stable)
    rank = (M_HEAD_DIM, M_HEAD_DIM)
    unit = (
        lax.broadcasted_iota(jnp.int32, rank, 0) == lax.broadcasted_iota(jnp.int32, rank, 1)
    ).astype(bf16)
    denoms = []
    for h in range(heads):
        lanes = slice(h * M_HEAD_DIM, (h + 1) * M_HEAD_DIM)
        query = sums[:, 0 * width :][:, lanes].astype(bf16)
        key = sums[:, 1 * width :][:, lanes].astype(bf16)
        value = sums[:, 2 * width :][:, lanes].astype(bf16)
        query_t[h] = lax.dot_general(unit, query, contract, preferred_element_type=f32)
        key_t[h] = lax.dot_general(unit, key, contract, preferred_element_type=f32) * scale
        value_rows[h] = value.astype(f32) * write[:, h : h + 1]
        keep_rows[h] = jnp.broadcast_to(keep[:, h : h + 1], (seq, M_HEAD_DIM))
        fresh = (
            keep[:, h : h + 1] * normalizer[:, h, :]
            + write[:, h : h + 1] * key.astype(f32) * scale
        )
        new_normalizer[:, h, :] = fresh
        denoms.append(jnp.sum(query.astype(f32) * fresh, axis=-1, keepdims=True))
    loads[4].wait()

    def one_head(h):
        for t in range(seq):
            fresh = (
                keep_rows[h, t : t + 1, :] * mem[t, h]
                + key_t[h, :, t : t + 1] * value_rows[h, t : t + 1, :]
            )
            mem[t, h] = fresh
            numer[h, t : t + 1, :] = jnp.sum(
                query_t[h, :, t : t + 1] * fresh, axis=0, keepdims=True
            )

    loop(0, heads, one_head)
    memory_store = pltpu.make_async_copy(mem, new_memory, store_sem.at[0])
    memory_store.start()
    outgate = sums[:, 3 * width : 4 * width].astype(bf16).astype(f32)
    opened = jax.nn.sigmoid(outgate)
    cells[me] = jnp.zeros(cells.shape[1:], bf16)
    for h in range(heads):
        lanes = slice(h * M_HEAD_DIM, (h + 1) * M_HEAD_DIM)
        hidden = numer[h] / jnp.maximum(jnp.abs(denoms[h]), 1.0)
        cells[me, pl.ds(0, seq), lanes] = (hidden * opened[:, lanes]).astype(bf16)

    def cell_copy(j, slot):
        own = cells.at[2 * slot + core]
        return remote(own, own, send_d.at[j], recv_d.at[slot], 2 * j + core)

    def cell_relay(slot, side):
        own = cells.at[2 * slot + side]
        return remote(own, own, relay_send.at[slot], relay_recv.at[slot], partner)

    loop(1, chips, lambda k: cell_copy(lax.rem(chip + k, chips), chip).start())
    cell_relay(chip, core).start()
    loads[5].wait()

    def relay_cell(k):
        slot = lax.rem(chip + chips - k, chips)
        cell_copy(slot, slot).wait_recv()
        cell_relay(slot, core).start()

    loop(1, chips, relay_cell)
    loop(0, chips, lambda slot: cell_relay(slot, 1 - core).wait_recv())
    mixes = jnp.dot(
        cells[...].reshape(n * 16, width), mix_w[...], preferred_element_type=f32
    ).astype(bf16)
    mixed_send[...] = mixes.reshape(n, 16, depth)

    def mixed_copy(to, slot):
        return remote(mixed_send.at[to], mixed.at[slot], send_e.at[to], recv_e.at[slot], to)

    loop(1, n, lambda k: mixed_copy(lax.rem(me + k, n), me).start())
    mixed[me] = mixed_send[me]

    group = (index[:, 0:1] >= group_width).astype(jnp.int32)
    lane = lax.broadcasted_iota(jnp.int32, (seq, LANES), 1)
    named = group * group_width + jnp.where(lane < HALF, lane, lane - HALF)
    inside = jnp.where(lane < HALF, lane, lane - HALF) < group_width
    shares = jnp.zeros((seq, LANES), f32)
    for k in range(top):
        hit = (index[:, k : k + 1] == named.astype(f32)) & inside
        shares = shares + jnp.where(hit, route_share[:, k : k + 1], 0.0)
    shares = split_lanes(shares)
    square = (seq, seq)
    earlier = (
        lax.broadcasted_iota(jnp.int32, square, 1) < lax.broadcasted_iota(jnp.int32, square, 0)
    ).astype(f32)
    second = group.astype(f32)
    before_second = jnp.dot(
        earlier, jnp.broadcast_to(second, (seq, LANES)), preferred_element_type=f32
    )[:, 0:1]
    order = lax.broadcasted_iota(jnp.int32, (seq, 1), 0).astype(f32)
    place = jnp.where(second > 0.5, before_second + slots, order - before_second)
    spread = (
        place == lax.broadcasted_iota(jnp.int32, (seq, 2 * slots), 1).astype(f32)
    ).astype(bf16)

    def wait_mixed(k):
        of = lax.rem(me + k, n)
        mixed_copy(of, of).wait_recv()

    loop(1, n, wait_mixed)
    for d in range(n):
        columns = slice(d * depth, (d + 1) * depth)
        resid_rows[:, columns] = tokens[:, columns].astype(f32) + mixed[
            d, pl.ds(0, seq), :
        ].astype(f32)
    resid = resid_rows[...]
    moe_in = rms_normed(resid, moe_gain[...]).astype(bf16)
    first = (((0,), (0,)), ((), ()))
    for g in range(2):
        mine = spread[:, g * slots : (g + 1) * slots]
        packed[g, :, :model] = lax.dot_general(
            mine, moe_in, first, preferred_element_type=f32
        ).astype(bf16)
        packed[g, :, model:] = lax.dot_general(
            mine, shares, first, preferred_element_type=f32
        ).astype(bf16)

    half_chips = chips // 2

    def route_copy(j, slot):
        return remote(
            packed.at[j // half_chips],
            routed.at[2 * slot + core],
            send_f.at[j],
            recv_f.at[slot],
            2 * j + core,
        )

    def relay_copy(slot, side):
        return remote(
            routed.at[2 * slot + side],
            routed.at[2 * slot + side],
            send_g.at[slot],
            recv_g.at[slot],
            partner,
        )

    loop(1, chips, lambda k: route_copy(lax.rem(chip + k, chips), chip).start())
    routed[me] = packed[chip // half_chips]
    relay_copy(chip, core).start()

    def relay(k):
        slot = lax.rem(chip + chips - k, chips)
        route_copy(slot, slot).wait_recv()
        relay_copy(slot, core).start()

    loop(1, chips, relay)
    for load in loads[6:]:
        load.wait()
    loop(0, chips, lambda slot: relay_copy(slot, 1 - core).wait_recv())

    arrived = routed[...].reshape(n * slots, model + LANES)
    rows = arrived[:, :model]
    gate = jnp.dot(rows, gate_e[0], preferred_element_type=f32)
    upward = jnp.dot(rows, up_e[0], preferred_element_type=f32)
    inner = (gate * jax.nn.sigmoid(gate) * upward).astype(bf16)
    spot = lax.rem(me, group_width)
    lane = lax.broadcasted_iota(jnp.int32, (n * slots, LANES), 1)
    share = jnp.sum(
        jnp.where(
            (lane == spot) | (lane == spot + HALF), arrived[:, model:].astype(f32), 0.0
        ),
        axis=1,
        keepdims=True,
    )
    result = jnp.dot(inner, down_e[0], preferred_element_type=f32).astype(bf16).astype(f32)
    outcome[...] = (result * share).reshape(n, slots, model)

    def back_pair(j):
        return remote(
            back_pair_send.at[j], back_pair_recv.at[j], send_h.at[j], recv_h.at[j], partner
        )

    def send_back_pair(k):
        j = lax.rem(chip + k, chips)
        back_pair_send[j] = outcome[2 * j + 1 - core].astype(bf16)
        back_pair(j).start()

    loop(1, chips + 1, send_back_pair)

    def back_copy(j, slot):
        return remote(
            back_send.at[j], back_recv.at[slot], send_i.at[j], recv_i.at[slot], 2 * j + core
        )

    def send_back(k):
        j = lax.rem(chip + k, chips)
        back_pair(j).wait()
        back_send[j] = (outcome[2 * j + core] + back_pair_recv[j].astype(f32)).astype(bf16)
        back_copy(j, chip).start()

    loop(1, chips, send_back)
    back_pair(chip).wait()
    back_recv[chip] = (outcome[me] + back_pair_recv[chip].astype(f32)).astype(bf16)

    def wait_back(k):
        j = lax.rem(chip + k, chips)
        back_copy(j, j).wait()

    loop(1, chips, wait_back)
    combined = resid
    for g in range(2):
        base = g * half_chips
        back = lax.fori_loop(
            1,
            half_chips,
            lambda j, carry: carry + back_recv[base + j].astype(f32),
            back_recv[base].astype(f32),
        )
        high = back.astype(bf16)
        low = (back - high.astype(f32)).astype(bf16)
        mine = spread[:, g * slots : (g + 1) * slots]
        combined = combined + jnp.dot(mine, high, preferred_element_type=f32)
        combined = combined + jnp.dot(mine, low, preferred_element_type=f32)
    layer_out[...] = combined.astype(bf16)

    def sent(k):
        to = lax.rem(me + k, n)
        mixed_copy(to, me).wait_send()

    loop(1, n, sent)
    loop(1, chips, lambda k: cell_copy(lax.rem(chip + k, chips), chip).wait_send())
    loop(0, chips, lambda slot: cell_relay(slot, core).wait_send())
    loop(1, chips, lambda k: route_copy(lax.rem(chip + k, chips), chip).wait_send())
    loop(0, chips, lambda slot: relay_copy(slot, core).wait_send())
    memory_store.wait()


def on_device(
    tokens,
    norm_gain,
    query_weight,
    key_weight,
    value_weight,
    outgate_weight,
    ingate_weight,
    forget_weight,
    ingate_bias,
    forget_bias,
    memory,
    normalizer,
    stabilizer,
    mixer_weight,
    moe_gain,
    expert_gate,
    expert_up,
    expert_down,
    expert_index,
    route_weights,
):
    n = lax.axis_size("ep")
    seq, model = tokens.shape
    depth, width = query_weight.shape
    heads = ingate_bias.shape[0]
    hidden = expert_gate.shape[2]
    chosen_k = expert_index.shape[1]
    group_width = n // 2
    capacity = max(2, ((seq + 1) // 2 * chosen_k + group_width - 1) // group_width)
    most = min(seq, group_width * capacity // chosen_k)
    slots = (most + 7) // 8 * 8
    chips = n // 2
    total = 4 * width + LANES
    tail = (total // LANES + 1) // 2 * LANES
    assert 8 < seq <= 12
    vmem = pl.BlockSpec(memory_space=pltpu.VMEM)
    hbm = pl.BlockSpec(memory_space=pl.ANY)
    dma = pltpu.SemaphoreType.DMA
    V = pltpu.VMEM
    wide, narrow = (n,), (chips,)
    return_shapes = (
        jax.ShapeDtypeStruct((seq, model), bf16),
        jax.ShapeDtypeStruct(normalizer.shape, f32),
        jax.ShapeDtypeStruct((heads, seq), f32),
        jax.ShapeDtypeStruct(memory.shape, f32),
    )
    out, norm_out, stab_out, mem_out = pl.pallas_call(
        functools.partial(layer_kernel, n, seq, group_width),
        out_shape=return_shapes,
        in_specs=[vmem] * 11 + [hbm] * 9,
        out_specs=(vmem, vmem, vmem, hbm),
        scratch_shapes=[
            V((32, LANES), f32),
            V((16, LANES), f32),
            V((depth, 4 * width), bf16),
            V((LANES, depth), f32),
            V(memory.shape, f32),
            V(mixer_weight.shape, bf16),
            V(expert_gate.shape, bf16),
            V(expert_up.shape, bf16),
            V(expert_down.shape, bf16),
            V((n, 16, depth), bf16),
            V((n, 16, depth), bf16),
            V((n, 16, total), f32),
            V((chips, 16, total), bf16),
            V((chips, 16, total), bf16),
            V((chips, 8, total + tail), bf16),
            V((chips, 8, total + tail), bf16),
            V((heads, M_HEAD_DIM, seq), f32),
            V((heads, M_HEAD_DIM, seq), f32),
            V((heads, seq, M_HEAD_DIM), f32),
            V((heads, seq, M_HEAD_DIM), f32),
            V((heads, seq, M_HEAD_DIM), f32),
            V((n, 16, width), bf16),
            V((n, 16, depth), bf16),
            V((n, 16, depth), bf16),
            V((seq, model), f32),
            V((2, slots, model + LANES), bf16),
            V((n, slots, model + LANES), bf16),
            V((n, slots, model), f32),
            V((chips, slots, model), bf16),
            V((chips, slots, model), bf16),
            V((chips, slots, model), bf16),
            V((chips, slots, model), bf16),
            dma((9,)),
            dma((1,)),
        ]
        + [dma(wide), dma(wide)]
        + [dma(narrow), dma(narrow)] * 4
        + [dma(wide), dma(wide)]
        + [dma(narrow), dma(narrow)] * 4,
        compiler_params=pltpu.CompilerParams(
            collective_id=0, has_side_effects=True, vmem_limit_bytes=60 * 1024 * 1024
        ),
    )(
        tokens,
        norm_gain.reshape(1, model),
        ingate_weight.T,
        forget_weight.T,
        ingate_bias.reshape(1, heads),
        forget_bias.reshape(1, heads),
        normalizer,
        stabilizer.T,
        moe_gain.reshape(1, model),
        expert_index.T,
        route_weights.T,
        query_weight,
        key_weight,
        value_weight,
        outgate_weight,
        memory,
        mixer_weight,
        expert_gate,
        expert_up,
        expert_down,
    )
    return (out, mem_out, norm_out, stab_out.T)


def solution(mesh):
    return jax.shard_map(
        on_device,
        mesh=mesh,
        in_specs=(
            P(("grp", "ep"), None),
            P(),
            P("ep", None),
            P("ep", None),
            P("ep", None),
            P("ep", None),
            P("ep", None),
            P("ep", None),
            P(),
            P(),
            P(("grp", "ep"), None, None, None),
            P(("grp", "ep"), None, None),
            P(("grp", "ep"), None),
            P(None, "ep"),
            P(),
            P("ep", None, None),
            P("ep", None, None),
            P("ep", None, None),
            P(("grp", "ep"), None),
            P(("grp", "ep"), None),
        ),
        out_specs=(
            P(("grp", "ep"), None),
            P(("grp", "ep"), None, None, None),
            P(("grp", "ep"), None, None),
            P(("grp", "ep"), None),
        ),
        check_vma=False,
    )
```

```python
import functools

import jax
import jax.numpy as jnp
from jax import lax
from jax.experimental import pallas as pl
from jax.experimental.pallas import tpu as pltpu
from jax.sharding import PartitionSpec as P

M_HEAD_DIM = 128
LANES = 128
HALF = 64
EPS = 1e-06
f32 = jnp.float32
bf16 = jnp.bfloat16


def rms_normed(values, gain):
    scale = lax.rsqrt(jnp.mean(values * values, axis=-1, keepdims=True) + EPS)
    return values * scale * gain


def remote(src, dst, send_sem, recv_sem, device):
    return pltpu.make_async_remote_copy(
        src_ref=src,
        dst_ref=dst,
        send_sem=send_sem,
        recv_sem=recv_sem,
        device_id={"ep": device},
        device_id_type=pl.DeviceIdType.MESH,
    )


def loop(low, high, body):
    def step(index, carry):
        body(index)
        return carry

    lax.fori_loop(low, high, step, 0)


def far_first(k, count):
    half = count // 2
    return half + (1 - 2 * lax.rem(k, 2)) * (k // 2)


def split_lanes(values):
    lane = lax.broadcasted_iota(jnp.int32, values.shape, 1)
    high = values.astype(bf16).astype(f32)
    return jnp.where(lane < HALF, high, values - high).astype(bf16)


def layer_kernel(
    n,
    seq,
    group_width,
    tokens,
    norm_gain,
    ingate_weight,
    forget_weight,
    ingate_bias,
    forget_bias,
    normalizer,
    stabilizer,
    moe_gain,
    expert_index,
    route_weights,
    query_weight,
    key_weight,
    value_weight,
    outgate_weight,
    memory,
    mixer_weight,
    expert_gate,
    expert_up,
    expert_down,
    layer_out,
    new_normalizer,
    new_stabilizer,
    new_memory,
    small,
    flip,
    proj_w,
    gate_w,
    mem,
    mix_w,
    gate_e,
    up_e,
    down_e,
    normed,
    normed_cols,
    part,
    pair_send,
    pair_recv,
    sum_send,
    sum_recv,
    key_t,
    query_t,
    value_rows,
    keep_rows,
    numer,
    cells,
    mixed_send,
    mixed,
    resid_rows,
    packed,
    routed,
    outcome,
    back_pair_send,
    back_pair_recv,
    back_send,
    back_recv,
    load_sem,
    send_a,
    recv_a,
    send_b,
    recv_b,
    send_c,
    recv_c,
    send_d,
    recv_d,
    relay_send,
    relay_recv,
    send_e,
    recv_e,
    send_f,
    recv_f,
    send_g,
    recv_g,
    send_h,
    recv_h,
    send_i,
    recv_i,
):
    me = lax.axis_index("ep")
    core = lax.rem(me, 2)
    chip = me // 2
    partner = me + 1 - 2 * core
    chips = n // 2
    width = proj_w.shape[1] // 4
    heads = mem.shape[1]
    model = tokens.shape[1]
    slots = packed.shape[1]
    total = part.shape[2]

    loads = [
        pltpu.make_async_copy(source, target, load_sem.at[index])
        for index, (source, target) in enumerate(
            (
                (query_weight, proj_w.at[:, pl.ds(0, width)]),
                (key_weight, proj_w.at[:, pl.ds(width, width)]),
                (value_weight, proj_w.at[:, pl.ds(2 * width, width)]),
                (outgate_weight, proj_w.at[:, pl.ds(3 * width, width)]),
                (memory, mem),
                (mixer_weight, mix_w),
                (expert_gate, gate_e),
                (expert_up, up_e),
                (expert_down, down_e),
            )
        )
    ]
    for load in loads:
        load.start()

    barrier = pltpu.get_barrier_semaphore()

    def greet(k):
        pl.semaphore_signal(
            barrier,
            inc=1,
            device_id={"ep": lax.rem(me + far_first(k, n), n)},
            device_id_type=pl.DeviceIdType.MESH,
        )

    loop(1, n, greet)

    stream = tokens[...].astype(f32)
    depth = normed_cols.shape[2]
    scaled = rms_normed(stream, norm_gain[...]).astype(bf16)
    normed[:, pl.ds(seq, 16 - seq), :] = jnp.zeros((n, 16 - seq, depth), bf16)
    for d in range(n):
        normed[d, pl.ds(0, seq), :] = scaled[:, d * depth : (d + 1) * depth]
    gate_w[...] = jnp.zeros(gate_w.shape, f32)
    for base in (0, HALF):
        gate_w[base : base + heads, :] = ingate_weight[...].astype(f32)
        gate_w[base + heads : base + 2 * heads, :] = forget_weight[...].astype(f32)
    top = expert_index.shape[0]
    small[...] = jnp.zeros(small.shape, f32)
    small[0:heads, 0:seq] = stabilizer[...]
    small[8 : 8 + top, 0:seq] = route_weights[...]
    small[16 : 16 + top, 0:seq] = expert_index[...].astype(f32)
    flipped = small[...].T
    old_stable = flipped[:seq, 0:heads]
    route_share = flipped[:seq, 8 : 8 + top]
    index = flipped[:seq, 16 : 16 + top]

    pl.semaphore_wait(barrier, n - 1)

    def send_cols(k):
        to = lax.rem(me + far_first(k, n), n)
        remote(normed.at[to], normed_cols.at[me], send_a.at[to], recv_a.at[me], to).start()

    def wait_cols(k):
        of = lax.rem(me + far_first(k, n), n)
        remote(normed.at[of], normed_cols.at[of], send_a.at[of], recv_a.at[of], of).wait()

    loop(1, n, send_cols)
    normed_cols[me] = normed[me]
    for load in loads[:4]:
        load.wait()
    loop(1, n, wait_cols)

    rows = normed_cols[...].reshape(n * 16, depth)
    for piece in range(4):
        columns = slice(piece * width, (piece + 1) * width)
        block = jnp.dot(rows, proj_w[:, columns], preferred_element_type=f32)
        part[:, :, columns] = block.reshape(n, 16, width)
    contract = (((1,), (1,)), ((), ()))
    gates = lax.dot_general(
        rows, gate_w[...].astype(bf16), contract, preferred_element_type=f32
    )
    part[:, :, 4 * width :] = gates.reshape(n, 16, LANES)

    def pack_sums(values):
        return values[:, : 4 * width].astype(bf16), split_lanes(values[:, 4 * width :])

    def unpack_sums(values):
        narrow = values[:, 4 * width :]
        whole = narrow + pltpu.roll(narrow, HALF, 1)
        return jnp.concatenate([values[:, : 4 * width], whole], axis=1)

    tail = sum_send.shape[2] - part.shape[2]

    def fold(values):
        rest = values[8:16]
        moved = pltpu.roll(rest[:, tail:], 4, 0)
        rest = jnp.concatenate(
            [rest[:, : total - tail] + moved, rest[:, total - tail : tail]], axis=1
        )
        return values[:8], rest

    def unfold(values):
        rest = values[:, total:]
        moved = pltpu.roll(rest[:, : total - tail], 4, 0)
        return jnp.concatenate(
            [values[:, :total], jnp.concatenate([rest, moved], axis=1)], axis=0
        )

    def pair_copy(j):
        return remote(
            pair_send.at[j], pair_recv.at[j], send_b.at[j], recv_b.at[j], partner
        )

    def send_pair(k):
        send_pair_of(lax.rem(chip + far_first(k, chips), chips))

    def send_pair_of(j):
        wide, narrow = pack_sums(part[2 * j + 1 - core])
        pair_send[j, :, : 4 * width] = wide
        pair_send[j, :, 4 * width :] = narrow
        pair_copy(j).start()

    loop(1, chips, send_pair)
    send_pair_of(chip)

    def sum_copy(j, slot):
        return remote(
            sum_send.at[j],
            sum_recv.at[slot],
            send_c.at[j],
            recv_c.at[slot],
            2 * j + core,
        )

    def send_sum(k):
        j = lax.rem(chip + far_first(k, chips), chips)
        pair_copy(j).wait()
        wide, narrow = pack_sums(part[2 * j + core] + unpack_sums(pair_recv[j].astype(f32)))
        joined = jnp.concatenate([wide.astype(f32), narrow.astype(f32)], axis=1)
        head, rest = fold(joined)
        sum_send[j, :, :total] = head.astype(bf16)
        sum_send[j, :, total:] = rest.astype(bf16)
        sum_copy(j, chip).start()

    loop(1, chips, send_sum)
    pair_copy(chip).wait()
    own = part[me] + unpack_sums(pair_recv[chip].astype(f32))

    def wait_sum(k, carry):
        j = lax.rem(chip + far_first(k, chips), chips)
        sum_copy(j, j).wait()
        return carry + sum_recv[j].astype(f32)

    others = lax.fori_loop(1, chips, wait_sum, jnp.zeros(sum_recv.shape[1:], f32))
    sums = (own + unpack_sums(unfold(others)))[:seq]

    scale = M_HEAD_DIM ** (-0.5)
    gates = sums[:, 4 * width : 4 * width + 2 * heads]
    ingate_pre = gates[:, :heads] + ingate_bias[...]
    forget_pre = gates[:, heads:] + forget_bias[...]
    log_forget = jnp.minimum(forget_pre, 0.0) - jnp.log1p(jnp.exp(-jnp.abs(forget_pre)))
    stable = jnp.maximum(log_forget + old_stable, ingate_pre)
    flip[...] = jnp.zeros(flip.shape, f32)
    flip[0:seq, 0:heads] = stable
    new_stabilizer[...] = flip[...].T[:heads, :seq]
    keep = jnp.exp(log_forget + old_stable - stable)
    write = jnp.exp(ingate_pre - stable)
    rank = (M_HEAD_DIM, M_HEAD_DIM)
    unit = (
        lax.broadcasted_iota(jnp.int32, rank, 0) == lax.broadcasted_iota(jnp.int32, rank, 1)
    ).astype(bf16)
    denoms = []
    for h in range(heads):
        lanes = slice(h * M_HEAD_DIM, (h + 1) * M_HEAD_DIM)
        query = sums[:, 0 * width :][:, lanes].astype(bf16)
        key = sums[:, 1 * width :][:, lanes].astype(bf16)
        value = sums[:, 2 * width :][:, lanes].astype(bf16)
        query_t[h] = lax.dot_general(unit, query, contract, preferred_element_type=f32)
        key_t[h] = lax.dot_general(unit, key, contract, preferred_element_type=f32) * scale
        value_rows[h] = value.astype(f32) * write[:, h : h + 1]
        keep_rows[h] = jnp.broadcast_to(keep[:, h : h + 1], (seq, M_HEAD_DIM))
        fresh = (
            keep[:, h : h + 1] * normalizer[:, h, :]
            + write[:, h : h + 1] * key.astype(f32) * scale
        )
        new_normalizer[:, h, :] = fresh
        denoms.append(jnp.sum(query.astype(f32) * fresh, axis=-1, keepdims=True))
    loads[4].wait()

    def one_head(h):
        for t in range(seq):
            fresh = (
                keep_rows[h, t : t + 1, :] * mem[t, h]
                + key_t[h, :, t : t + 1] * value_rows[h, t : t + 1, :]
            )
            new_memory[t, h] = fresh
            numer[h, t : t + 1, :] = jnp.sum(
                query_t[h, :, t : t + 1] * fresh, axis=0, keepdims=True
            )

    loop(0, heads, one_head)
    outgate = sums[:, 3 * width : 4 * width].astype(bf16).astype(f32)
    opened = jax.nn.sigmoid(outgate)
    cells[me] = jnp.zeros(cells.shape[1:], bf16)
    for h in range(heads):
        lanes = slice(h * M_HEAD_DIM, (h + 1) * M_HEAD_DIM)
        hidden = numer[h] / jnp.maximum(jnp.abs(denoms[h]), 1.0)
        cells[me, pl.ds(0, seq), lanes] = (hidden * opened[:, lanes]).astype(bf16)

    def cell_copy(j, slot):
        own = cells.at[2 * slot + core]
        return remote(own, own, send_d.at[j], recv_d.at[slot], 2 * j + core)

    def cell_relay(slot, side):
        own = cells.at[2 * slot + side]
        return remote(own, own, relay_send.at[slot], relay_recv.at[slot], partner)

    loop(1, chips, lambda k: cell_copy(lax.rem(chip + far_first(k, chips), chips), chip).start())
    cell_relay(chip, core).start()
    loads[5].wait()

    def relay_cell(k):
        slot = lax.rem(chip + chips - far_first(k, chips), chips)
        cell_copy(slot, slot).wait_recv()
        cell_relay(slot, core).start()

    loop(1, chips, relay_cell)
    loop(0, chips, lambda slot: cell_relay(slot, 1 - core).wait_recv())
    mixes = jnp.dot(
        cells[...].reshape(n * 16, width), mix_w[...], preferred_element_type=f32
    ).astype(bf16)
    mixed_send[...] = mixes.reshape(n, 16, depth)

    def mixed_copy(to, slot):
        return remote(mixed_send.at[to], mixed.at[slot], send_e.at[to], recv_e.at[slot], to)

    loop(1, n, lambda k: mixed_copy(lax.rem(me + far_first(k, n), n), me).start())
    mixed[me] = mixed_send[me]

    group = (index[:, 0:1] >= group_width).astype(jnp.int32)
    lane = lax.broadcasted_iota(jnp.int32, (seq, LANES), 1)
    named = group * group_width + jnp.where(lane < HALF, lane, lane - HALF)
    inside = jnp.where(lane < HALF, lane, lane - HALF) < group_width
    shares = jnp.zeros((seq, LANES), f32)
    for k in range(top):
        hit = (index[:, k : k + 1] == named.astype(f32)) & inside
        shares = shares + jnp.where(hit, route_share[:, k : k + 1], 0.0)
    shares = split_lanes(shares)
    square = (seq, seq)
    earlier = (
        lax.broadcasted_iota(jnp.int32, square, 1) < lax.broadcasted_iota(jnp.int32, square, 0)
    ).astype(f32)
    second = group.astype(f32)
    before_second = jnp.dot(
        earlier, jnp.broadcast_to(second, (seq, LANES)), preferred_element_type=f32
    )[:, 0:1]
    order = lax.broadcasted_iota(jnp.int32, (seq, 1), 0).astype(f32)
    place = jnp.where(second > 0.5, before_second + slots, order - before_second)
    spread = (
        place == lax.broadcasted_iota(jnp.int32, (seq, 2 * slots), 1).astype(f32)
    ).astype(bf16)

    def wait_mixed(k):
        of = lax.rem(me + far_first(k, n), n)
        mixed_copy(of, of).wait_recv()

    loop(1, n, wait_mixed)
    for d in range(n):
        columns = slice(d * depth, (d + 1) * depth)
        resid_rows[:, columns] = tokens[:, columns].astype(f32) + mixed[
            d, pl.ds(0, seq), :
        ].astype(f32)
    resid = resid_rows[...]
    moe_in = rms_normed(resid, moe_gain[...]).astype(bf16)
    first = (((0,), (0,)), ((), ()))
    for g in range(2):
        mine = spread[:, g * slots : (g + 1) * slots]
        packed[g, :, :model] = lax.dot_general(
            mine, moe_in, first, preferred_element_type=f32
        ).astype(bf16)
        packed[g, :, model:] = lax.dot_general(
            mine, shares, first, preferred_element_type=f32
        ).astype(bf16)

    half_chips = chips // 2

    def route_copy(j, slot):
        return remote(
            packed.at[j // half_chips],
            routed.at[2 * slot + core],
            send_f.at[j],
            recv_f.at[slot],
            2 * j + core,
        )

    def relay_copy(slot, side):
        return remote(
            routed.at[2 * slot + side],
            routed.at[2 * slot + side],
            send_g.at[slot],
            recv_g.at[slot],
            partner,
        )

    loop(1, chips, lambda k: route_copy(lax.rem(chip + far_first(k, chips), chips), chip).start())
    routed[me] = packed[chip // half_chips]
    relay_copy(chip, core).start()

    def relay(k):
        slot = lax.rem(chip + chips - far_first(k, chips), chips)
        route_copy(slot, slot).wait_recv()
        relay_copy(slot, core).start()

    loop(1, chips, relay)
    for load in loads[6:]:
        load.wait()
    loop(0, chips, lambda slot: relay_copy(slot, 1 - core).wait_recv())

    arrived = routed[...].reshape(n * slots, model + LANES)
    rows = arrived[:, :model]
    gate = jnp.dot(rows, gate_e[0], preferred_element_type=f32)
    upward = jnp.dot(rows, up_e[0], preferred_element_type=f32)
    inner = (gate * jax.nn.sigmoid(gate) * upward).astype(bf16)
    spot = lax.rem(me, group_width)
    lane = lax.broadcasted_iota(jnp.int32, (n * slots, LANES), 1)
    share = jnp.sum(
        jnp.where(
            (lane == spot) | (lane == spot + HALF), arrived[:, model:].astype(f32), 0.0
        ),
        axis=1,
        keepdims=True,
    )
    result = jnp.dot(inner, down_e[0], preferred_element_type=f32).astype(bf16).astype(f32)
    outcome[...] = (result * share).reshape(n, slots, model)

    def back_pair(j):
        return remote(
            back_pair_send.at[j], back_pair_recv.at[j], send_h.at[j], recv_h.at[j], partner
        )

    def send_back_pair(k):
        send_back_pair_of(lax.rem(chip + far_first(k, chips), chips))

    def send_back_pair_of(j):
        back_pair_send[j] = outcome[2 * j + 1 - core].astype(bf16)
        back_pair(j).start()

    loop(1, chips, send_back_pair)
    send_back_pair_of(chip)

    def back_copy(j, slot):
        return remote(
            back_send.at[j], back_recv.at[slot], send_i.at[j], recv_i.at[slot], 2 * j + core
        )

    def send_back(k):
        j = lax.rem(chip + far_first(k, chips), chips)
        back_pair(j).wait()
        back_send[j] = (outcome[2 * j + core] + back_pair_recv[j].astype(f32)).astype(bf16)
        back_copy(j, chip).start()

    loop(1, chips, send_back)
    back_pair(chip).wait()
    back_recv[chip] = (outcome[me] + back_pair_recv[chip].astype(f32)).astype(bf16)

    def wait_back(k):
        j = lax.rem(chip + far_first(k, chips), chips)
        back_copy(j, j).wait()

    loop(1, chips, wait_back)
    combined = resid
    for g in range(2):
        base = g * half_chips
        back = lax.fori_loop(
            1,
            half_chips,
            lambda j, carry: carry + back_recv[base + j].astype(f32),
            back_recv[base].astype(f32),
        )
        high = back.astype(bf16)
        low = (back - high.astype(f32)).astype(bf16)
        mine = spread[:, g * slots : (g + 1) * slots]
        combined = combined + jnp.dot(mine, high, preferred_element_type=f32)
        combined = combined + jnp.dot(mine, low, preferred_element_type=f32)
    layer_out[...] = combined.astype(bf16)

    def sent(k):
        to = lax.rem(me + far_first(k, n), n)
        mixed_copy(to, me).wait_send()

    loop(1, n, sent)
    loop(1, chips, lambda k: cell_copy(lax.rem(chip + far_first(k, chips), chips), chip).wait_send())
    loop(0, chips, lambda slot: cell_relay(slot, core).wait_send())
    loop(1, chips, lambda k: route_copy(lax.rem(chip + far_first(k, chips), chips), chip).wait_send())
    loop(0, chips, lambda slot: relay_copy(slot, core).wait_send())


def on_device(
    tokens,
    norm_gain,
    query_weight,
    key_weight,
    value_weight,
    outgate_weight,
    ingate_weight,
    forget_weight,
    ingate_bias,
    forget_bias,
    memory,
    normalizer,
    stabilizer,
    mixer_weight,
    moe_gain,
    expert_gate,
    expert_up,
    expert_down,
    expert_index,
    route_weights,
):
    n = lax.axis_size("ep")
    seq, model = tokens.shape
    depth, width = query_weight.shape
    heads = ingate_bias.shape[0]
    hidden = expert_gate.shape[2]
    chosen_k = expert_index.shape[1]
    group_width = n // 2
    capacity = max(2, ((seq + 1) // 2 * chosen_k + group_width - 1) // group_width)
    most = min(seq, group_width * capacity // chosen_k)
    slots = (most + 7) // 8 * 8
    chips = n // 2
    total = 4 * width + LANES
    tail = (total // LANES + 1) // 2 * LANES
    assert 8 < seq <= 12
    vmem = pl.BlockSpec(memory_space=pltpu.VMEM)
    hbm = pl.BlockSpec(memory_space=pltpu.HBM)
    dma = pltpu.SemaphoreType.DMA
    V = pltpu.VMEM
    wide, narrow = (n,), (chips,)
    return_shapes = (
        pltpu.VMEM((seq, model), bf16),
        pltpu.VMEM(normalizer.shape, f32),
        pltpu.VMEM((heads, seq), f32),
        pltpu.VMEM(memory.shape, f32),
    )
    out, norm_out, stab_out, mem_out = pl.pallas_call(
        functools.partial(layer_kernel, n, seq, group_width),
        out_shape=return_shapes,
        in_specs=[vmem] * 11 + [hbm] * 9,
        out_specs=(vmem, vmem, vmem, vmem),
        scratch_shapes=[
            V((32, LANES), f32),
            V((16, LANES), f32),
            V((depth, 4 * width), bf16),
            V((LANES, depth), f32),
            V(memory.shape, f32),
            V(mixer_weight.shape, bf16),
            V(expert_gate.shape, bf16),
            V(expert_up.shape, bf16),
            V(expert_down.shape, bf16),
            V((n, 16, depth), bf16),
            V((n, 16, depth), bf16),
            V((n, 16, total), f32),
            V((chips, 16, total), bf16),
            V((chips, 16, total), bf16),
            V((chips, 8, total + tail), bf16),
            V((chips, 8, total + tail), bf16),
            V((heads, M_HEAD_DIM, seq), f32),
            V((heads, M_HEAD_DIM, seq), f32),
            V((heads, seq, M_HEAD_DIM), f32),
            V((heads, seq, M_HEAD_DIM), f32),
            V((heads, seq, M_HEAD_DIM), f32),
            V((n, 16, width), bf16),
            V((n, 16, depth), bf16),
            V((n, 16, depth), bf16),
            V((seq, model), f32),
            V((2, slots, model + LANES), bf16),
            V((n, slots, model + LANES), bf16),
            V((n, slots, model), f32),
            V((chips, slots, model), bf16),
            V((chips, slots, model), bf16),
            V((chips, slots, model), bf16),
            V((chips, slots, model), bf16),
            dma((9,)),
        ]
        + [dma(wide), dma(wide)]
        + [dma(narrow), dma(narrow)] * 4
        + [dma(wide), dma(wide)]
        + [dma(narrow), dma(narrow)] * 4,
        compiler_params=pltpu.CompilerParams(
            collective_id=0, has_side_effects=True, vmem_limit_bytes=54 * 1024 * 1024
        ),
    )(
        tokens,
        norm_gain.reshape(1, model),
        ingate_weight.T,
        forget_weight.T,
        ingate_bias.reshape(1, heads),
        forget_bias.reshape(1, heads),
        normalizer,
        stabilizer.T,
        moe_gain.reshape(1, model),
        expert_index.T,
        route_weights.T,
        query_weight,
        key_weight,
        value_weight,
        outgate_weight,
        memory,
        mixer_weight,
        expert_gate,
        expert_up,
        expert_down,
    )
    return (out, mem_out, norm_out, stab_out.T)


def solution(mesh):
    return jax.shard_map(
        on_device,
        mesh=mesh,
        in_specs=(
            P(("grp", "ep"), None),
            P(),
            P("ep", None),
            P("ep", None),
            P("ep", None),
            P("ep", None),
            P("ep", None),
            P("ep", None),
            P(),
            P(),
            P(("grp", "ep"), None, None, None),
            P(("grp", "ep"), None, None),
            P(("grp", "ep"), None),
            P(None, "ep"),
            P(),
            P("ep", None, None),
            P("ep", None, None),
            P("ep", None, None),
            P(("grp", "ep"), None),
            P(("grp", "ep"), None),
        ),
        out_specs=(
            P(("grp", "ep"), None),
            P(("grp", "ep"), None, None, None),
            P(("grp", "ep"), None, None),
            P(("grp", "ep"), None),
        ),
        check_vma=False,
    )
```
